32 devices in a mesh: fs: 8 (over z, y), tp: 4 (over x, core).
Axes of the slice: x: 2, y: 2, z: 4, core: 2. Of those that a mesh axis runs over, the one named last changes fastest.
Arguments:
- tokens: bfloat16 [8192, 2048], P('fs'), may hold values from -6 to 6
- norm_gain: float32 [2048], P('fs'), may hold values from 0.1 to 1.9
- gate_train: float32 [8, 2048, 768], P(None, 'fs', 'tp'), may hold values from -0.125 to 0.125
- up_train: float32 [8, 2048, 768], P(None, 'fs', 'tp'), may hold values from -0.125 to 0.125
- down_train: float32 [8, 768, 2048], P(None, 'fs', 'tp'), may hold values from -0.21875 to 0.21875
- expert_ids: int32 [8192, 2], P('fs'), may hold values from 0 to 7, all different within a row; in each aligned block of 1024 rows (0 to 1023, 1024 to 2047, ...) at most 512 rows name the same one
- route_weights: float32 [8192, 2], P('fs'), may hold values from 0.1 to 1
Outputs:
- gate_serve: bfloat16 [8, 2048, 768], P('fs', None, 'tp')
- up_serve: bfloat16 [8, 2048, 768], P('fs', None, 'tp')
- down_serve: bfloat16 [8, 768, 2048], P('fs', 'tp')
- mixed: bfloat16 [8192, 2048], P('fs', 'tp')
The draws below stay inside these ranges and needn't reach their ends.
Inputs may be any that keep to these rules, and one draw needn't show every extreme that they name: `expert_ids`: each row names 2 different experts. Within each aligned block of 1024 rows no expert is named more than 512 times, and in every block some expert is named exactly 512 times; every expert is named somewhere.
All inputs are finite; a program needn't handle non-finite values.
Results may differ from the reference program's by a relative error of at most 0.011.
Values may be sent and summed in bfloat16 or wider, within the bound.
A program may use at most 128 MiB of HBM per device.

```python
import math
import jax
import jax.numpy as jnp
import numpy as np
from jax import lax

D = 2048
FF = 768
TOP = 2
TOK_DEV = 1024
EXPERTS = 8
CAP = 512
TOKENS = 8192
N_FS = 8
N_TP = 4


def shard_levels(key, shape, shards, least, top_value):
    loudness = 1.0
    for axis_at, parts in shards:
        draws = jax.random.uniform(jax.random.fold_in(jax.random.fold_in(key, 6), axis_at), (parts,), jnp.float32, least / len(shards), top_value / len(shards))
        loudness = loudness * jnp.repeat(jnp.exp(draws), shape[axis_at] // parts).reshape((-1,) + (1,) * (len(shape) - 1 - axis_at))
    return loudness


def shared_out(own_key, own, number, rows, number_of, top, limit, lean):
    ranking = jax.random.permutation(own_key, number_of)
    heavy_load, ordinary = portions_of(number_of, rows * top, limit, lean, True), portions_of(number_of, rows * top, limit, lean, False)
    places = jnp.arange(number_of)

    def named(sizes, offset_by):
        used = int((sizes > 0).sum())
        fixed = max(1, used // 4)
        moved = fixed + (places - fixed + offset_by * (used - fixed)) % max(1, number_of - fixed)
        return jnp.zeros((number_of,), jnp.int32).at[ranking[jnp.where(places < fixed, places, moved)]].set(jnp.asarray(sizes, jnp.int32))

    sizes = jnp.where(number % 4 == 0, named(heavy_load, number // 4), named(ordinary, number - number // 4 - 1))
    mixed = jax.random.permutation(jax.random.fold_in(own, 3), number_of)
    source_of, sink = mixed[0:number_of // 2 * 2:2], mixed[1:number_of // 2 * 2:2]
    slack = jnp.minimum(sizes[source_of] - 1, limit - sizes[sink]) // 2
    slack = jnp.where((source_of == ranking[0]) | (sink == ranking[0]) | (sizes[sink] == 0), 0, jnp.maximum(slack, 0))
    moved = jax.random.randint(jax.random.fold_in(own, 4), (number_of // 2,), 0, 1 << 20) % (slack + 1)
    sizes = sizes.at[source_of].add(-moved).at[sink].add(moved)
    items = jnp.searchsorted(jnp.cumsum(sizes), jnp.arange(rows * top), side="right").astype(jnp.int32)
    table = items.reshape(top, rows).T
    table = table[jax.random.permutation(jax.random.fold_in(own, 1), rows)]
    offset_by = jax.random.randint(jax.random.fold_in(own, 2), (rows, 1), 0, top)
    return jnp.take_along_axis(table, (jnp.arange(top)[None, :] + offset_by) % top, axis=1)


def portions_of(number_of, total, limit, slope, full):
    portions = [(1 << 20) // math.isqrt(standing ** slope) + 1 for standing in range(1, number_of + 1)]
    largest = limit if full else min(limit, max(-(-total // number_of), total * portions[0] // sum(portions)))
    least = 1 if total - largest >= number_of - 1 else 0
    counts, rest = [largest] + [least] * (number_of - 1), total - largest - least * (number_of - 1)
    while rest > 0:
        movable = [i for i in range(1, number_of) if counts[i] < largest] or [i for i in range(1, number_of) if counts[i] < limit]
        mass, budget = sum([portions[i] for i in movable]), rest
        for i in movable:
            addition = min(limit - counts[i], max(1, budget * portions[i] // mass), rest)
            counts[i] = counts[i] + addition
            rest = rest - addition
    return np.array(counts)


def bell_draw(rng, dims, spread, reach, pieces=(), held_as=jnp.bfloat16):
    entries = jax.random.normal(rng, dims, jnp.float32) * spread
    if len(pieces) > 0:
        entries = shard_levels(rng, dims, pieces, -0.22, 0.18) * entries
    return jnp.clip(entries, min=-reach, max=reach).astype(held_as)


def setup_inputs(seed: int = 0) -> dict:
    keys = jax.random.split(jax.random.key(seed), 8)
    tokens = bell_draw(keys[0], (TOKENS, D), 1.0, 6.0, ((0, 8),))
    norm_gain = jnp.clip(1.0 + 0.18 * jax.random.normal(keys[1], (D,), jnp.float32), 0.1, 1.9)
    gate_train = bell_draw(keys[2], (EXPERTS, D, FF), D ** -0.5, 0.125, ((1, 8), (2, 4)), jnp.float32)
    up_train = bell_draw(keys[3], (EXPERTS, D, FF), D ** -0.5, 0.125, ((1, 8), (2, 4)), jnp.float32)
    down_train = bell_draw(keys[4], (EXPERTS, FF, D), FF ** -0.5, 0.21875, ((1, 8), (2, 4)), jnp.float32)
    expert_ids_keys = jax.random.split(jax.random.fold_in(keys[5], 1), TOKENS // TOK_DEV)
    expert_ids_turns = jax.random.permutation(jax.random.fold_in(keys[5], 3), TOKENS // TOK_DEV)
    expert_ids = jax.vmap(lambda own, number: shared_out(jax.random.fold_in(keys[5], 2), own, number, TOK_DEV, EXPERTS, TOP, CAP, 2))(expert_ids_keys, expert_ids_turns).reshape((TOKENS, TOP))
    route_weights = jnp.clip(jnp.exp(math.log(1.0) - 2.3025851 * jax.random.uniform(keys[6], (TOKENS, TOP), jnp.float32) ** shard_levels(keys[6], (TOKENS, TOP), ((0, 8),), -0.2, 0.2)), 0.1, 1.0)
    return dict(tokens=tokens, norm_gain=norm_gain, gate_train=gate_train, up_train=up_train, down_train=down_train, expert_ids=expert_ids, route_weights=route_weights)


epsilon = 1e-06

def reference(tokens, norm_gain, gate_train, up_train, down_train, expert_ids, route_weights):
    gate_serve = (norm_gain[None, :, None] * gate_train).astype(jnp.bfloat16)
    up_serve = (norm_gain[None, :, None] * up_train).astype(jnp.bfloat16)
    down_serve = down_train.astype(jnp.bfloat16)
    tok_float = tokens.astype(jnp.float32)
    normed = (tok_float * lax.rsqrt(lax.optimization_barrier(jnp.mean(tok_float * tok_float, axis=-1, keepdims=True)) + epsilon)).astype(jnp.bfloat16)
    flat_ids = expert_ids.reshape(N_FS, TOK_DEV * TOP)
    onehot = (flat_ids[:, :, None] == jnp.arange(EXPERTS, dtype=jnp.int32)[None, None, :]).astype(jnp.int32)
    slot_rank = lax.optimization_barrier(jnp.sum((jnp.cumsum(onehot, axis=1) - onehot) * onehot, axis=-1))
    row_index = (jnp.arange(N_FS, dtype=jnp.int32)[:, None] * CAP + slot_rank).astype(jnp.int32)
    tok_index = (jnp.arange(N_FS, dtype=jnp.int32)[:, None] * TOK_DEV + jnp.arange(TOK_DEV * TOP, dtype=jnp.int32)[None, :] // TOP).astype(jnp.int32)
    buffer = jnp.zeros((EXPERTS, N_FS * CAP, D), jnp.bfloat16)
    buffer = buffer.at[flat_ids.reshape(-1), row_index.reshape(-1)].set(normed[tok_index.reshape(-1)])
    block_width = FF // N_TP

    def expert_apply(inputs):
        routed, weight_gate, weight_up, weight_down = inputs
        gate_act = jnp.dot(routed, weight_gate, preferred_element_type=jnp.float32)
        up_act = jnp.dot(routed, weight_up, preferred_element_type=jnp.float32)
        hidden = (jax.nn.silu(gate_act) * up_act).astype(jnp.bfloat16)
        running = jnp.zeros((routed.shape[0], D), jnp.float32)
        for index_tp in range(N_TP):
            partial_value = jnp.dot(hidden[:, index_tp * block_width:(index_tp + 1) * block_width], weight_down[index_tp * block_width:(index_tp + 1) * block_width], preferred_element_type=jnp.float32)
            running = running + partial_value.astype(jnp.bfloat16).astype(jnp.float32)
        return running.astype(jnp.bfloat16)
    outputs = lax.map(expert_apply, (buffer, gate_serve, up_serve, down_serve))
    picked = outputs[flat_ids.reshape(-1), row_index.reshape(-1)].reshape(TOKENS, TOP, D).astype(jnp.float32)
    shares = route_weights / lax.optimization_barrier(jnp.sum(route_weights, axis=-1, keepdims=True))
    mixed = lax.optimization_barrier(jnp.sum(shares[:, :, None] * picked, axis=1)).astype(jnp.bfloat16)
    return (gate_serve, up_serve, down_serve, mixed)
```

```python
import jax
import jax.numpy as jnp
from jax import lax
from jax.sharding import PartitionSpec as P

epsilon = 1e-06


def on_device(tokens, norm_gain, gate_train, up_train, down_train, expert_ids, route_weights):
    experts, rows, cols = gate_train.shape
    fs_at = lax.axis_index("fs")
    tok_rows, picks = expert_ids.shape
    down_rows, down_cols = down_train.shape[1:]
    fs_count = lax.axis_size("fs")

    gate_up = jnp.concatenate(
        [norm_gain[None, :, None] * gate_train, norm_gain[None, :, None] * up_train], axis=2
    ).astype(jnp.bfloat16)
    gate_up = gate_up.transpose(1, 0, 2).reshape(rows, experts * 2 * cols)
    gate_up_all = lax.all_gather(gate_up, "fs", axis=0, tiled=True)
    down_all = lax.all_gather(
        down_train.astype(jnp.bfloat16).reshape(experts * down_rows, down_cols),
        "fs", axis=0, tiled=True,
    )

    tok_float = tokens.astype(jnp.float32)
    normed = (
        tok_float * lax.rsqrt(jnp.mean(tok_float * tok_float, axis=-1, keepdims=True) + epsilon)
    ).astype(jnp.bfloat16)
    shares = route_weights / jnp.sum(route_weights, axis=-1, keepdims=True)

    group = 2 * lax.axis_size("tp")
    picked = [jnp.zeros((tok_rows, cols), jnp.float32) for _ in range(picks)]
    for first in range(0, experts, group):
        part = gate_up_all[:, first * 2 * cols : (first + group) * 2 * cols]
        if first:
            part, picked = lax.optimization_barrier((part, picked))
        acts = jnp.dot(normed, part, preferred_element_type=jnp.float32)
        for at in range(group):
            g = acts[:, at * 2 * cols : at * 2 * cols + cols]
            u = acts[:, at * 2 * cols + cols : (at + 1) * 2 * cols]
            h = jax.nn.silu(g) * u
            for k in range(picks):
                picked[k] = picked[k] + jnp.where(
                    expert_ids[:, k : k + 1] == first + at, h, 0.0
                )
    hidden = jnp.stack([picked[k] * shares[:, k : k + 1] for k in range(picks)], 0)
    hidden_all = lax.all_gather(hidden.astype(jnp.bfloat16), "tp", axis=2, tiled=True)
    hidden_all = hidden_all.reshape(picks, tok_rows, fs_count, 1, down_rows)
    ids = jnp.arange(experts, dtype=jnp.int32)[None, None, :, None]
    mixed = jnp.zeros((tok_rows, down_cols), jnp.float32)
    for first in range(0, fs_count, group):
        blocks = hidden_all[:, :, first : first + group]
        if first:
            blocks, mixed = lax.optimization_barrier((blocks, mixed))
        spread = jnp.zeros((tok_rows, group, experts, down_rows), jnp.bfloat16)
        for k in range(picks):
            spread = jnp.where(expert_ids[:, k][:, None, None, None] == ids, blocks[k], spread)
        depth = experts * down_rows
        mixed = mixed + jnp.dot(
            spread.reshape(tok_rows, group * depth),
            down_all[first * depth : (first + group) * depth],
            preferred_element_type=jnp.float32,
        )
    mixed = mixed.astype(jnp.bfloat16)

    own = lax.dynamic_slice_in_dim(gate_up_all, fs_at * 2 * cols, 2 * cols, 1)
    down_own = lax.dynamic_slice_in_dim(
        down_all.reshape(fs_count, experts, down_rows, down_cols), fs_at, 1, 1
    ).reshape(1, fs_count * down_rows, down_cols)
    down_serve = lax.all_to_all(down_own, "tp", split_axis=1, concat_axis=2, tiled=True)
    return own[None, :, :cols], own[None, :, cols:], down_serve, mixed


def solution(mesh):
    return jax.shard_map(
        on_device,
        mesh=mesh,
        in_specs=(
            P("fs", None),
            P("fs"),
            P(None, "fs", "tp"),
            P(None, "fs", "tp"),
            P(None, "fs", "tp"),
            P("fs", None),
            P("fs", None),
        ),
        out_specs=(P("fs", None, "tp"), P("fs", None, "tp"), P("fs", "tp", None), P("fs", "tp")),
        check_vma=False,
    )
```

```python
import functools

import jax
import jax.numpy as jnp
from jax import lax
from jax.experimental import pallas as pl
from jax.experimental.pallas import tpu as pltpu
from jax.sharding import PartitionSpec as P

epsilon = 1e-06


def gathered(tokens, norm_gain, gate_train, up_train, down_train, expert_ids, route_weights):
    experts, rows, cols = gate_train.shape
    fs_at = lax.axis_index("fs")
    tok_rows, picks = expert_ids.shape
    down_rows, down_cols = down_train.shape[1:]
    fs_count = lax.axis_size("fs")

    gate_up = jnp.concatenate(
        [norm_gain[None, :, None] * gate_train, norm_gain[None, :, None] * up_train], axis=2
    ).astype(jnp.bfloat16)
    gate_up = gate_up.transpose(1, 0, 2).reshape(rows, experts * 2 * cols)
    gate_up_all = lax.all_gather(gate_up, "fs", axis=0, tiled=True)
    down_all = lax.all_gather(
        down_train.astype(jnp.bfloat16).reshape(experts * down_rows, down_cols),
        "fs", axis=0, tiled=True,
    )

    tok_float = tokens.astype(jnp.float32)
    normed = (
        tok_float * lax.rsqrt(jnp.mean(tok_float * tok_float, axis=-1, keepdims=True) + epsilon)
    ).astype(jnp.bfloat16)
    shares = route_weights / jnp.sum(route_weights, axis=-1, keepdims=True)

    group = 2 * lax.axis_size("tp")
    picked = [jnp.zeros((tok_rows, cols), jnp.float32) for _ in range(picks)]
    for first in range(0, experts, group):
        part = gate_up_all[:, first * 2 * cols : (first + group) * 2 * cols]
        if first:
            part, picked = lax.optimization_barrier((part, picked))
        acts = jnp.dot(normed, part, preferred_element_type=jnp.float32)
        for at in range(group):
            g = acts[:, at * 2 * cols : at * 2 * cols + cols]
            u = acts[:, at * 2 * cols + cols : (at + 1) * 2 * cols]
            h = jax.nn.silu(g) * u
            for k in range(picks):
                picked[k] = picked[k] + jnp.where(
                    expert_ids[:, k : k + 1] == first + at, h, 0.0
                )
    hidden = jnp.stack([picked[k] * shares[:, k : k + 1] for k in range(picks)], 0)
    hidden_all = lax.all_gather(hidden.astype(jnp.bfloat16), "tp", axis=2, tiled=True)
    hidden_all = hidden_all.reshape(picks, tok_rows, fs_count, 1, down_rows)
    ids = jnp.arange(experts, dtype=jnp.int32)[None, None, :, None]
    mixed = jnp.zeros((tok_rows, down_cols), jnp.float32)
    for first in range(0, fs_count, group):
        blocks = hidden_all[:, :, first : first + group]
        if first:
            blocks, mixed = lax.optimization_barrier((blocks, mixed))
        spread = jnp.zeros((tok_rows, group, experts, down_rows), jnp.bfloat16)
        for k in range(picks):
            spread = jnp.where(expert_ids[:, k][:, None, None, None] == ids, blocks[k], spread)
        depth = experts * down_rows
        mixed = mixed + jnp.dot(
            spread.reshape(tok_rows, group * depth),
            down_all[first * depth : (first + group) * depth],
            preferred_element_type=jnp.float32,
        )
    mixed = mixed.astype(jnp.bfloat16)

    own = lax.dynamic_slice_in_dim(gate_up_all, fs_at * 2 * cols, 2 * cols, 1)
    down_own = lax.dynamic_slice_in_dim(
        down_all.reshape(fs_count, experts, down_rows, down_cols), fs_at, 1, 1
    ).reshape(1, fs_count * down_rows, down_cols)
    down_serve = lax.all_to_all(down_own, "tp", split_axis=1, concat_axis=2, tiled=True)
    return own[None, :, :cols], own[None, :, cols:], down_serve, mixed


def ring_kernel(
    n, tp_count, blocks, gu_ref, dn_ref, normed_ref, ids_ref, shares_ref,
    main_ref, tail_ref, serve_ref, mixed_ref,
    gu_all, dn_all, picked, picked_all, total,
    send_sem, recv_sem, pick_send, pick_recv, serve_send, serve_recv, serve_copy, own_sem,
):
    fs_at, tp_at = lax.axis_index("fs"), lax.axis_index("tp")
    experts, down_rows, down_cols = dn_ref.shape
    rows = gu_ref.shape[1]
    tok_rows = normed_ref.shape[0]
    half = experts // 2
    last = n // 2

    place = (1 - fs_at % 2) * (fs_at // 2) + (fs_at % 2) * (n - 1 - fs_at // 2)

    def index_at(step):
        at = (place + step + n) % n
        odd = at // last
        return (1 - odd) * (2 * at) + odd * (2 * (n - 1 - at) + 1)

    right, left = index_at(1), index_at(-1)
    barrier = pltpu.get_barrier_semaphore()
    for to in (right, left):
        pl.semaphore_signal(
            barrier, inc=1, device_id={"fs": to}, device_id_type=pl.DeviceIdType.MESH
        )
    for hop in range(1, tp_count):
        pl.semaphore_signal(
            barrier, inc=1, device_id={"tp": (tp_at + hop) % tp_count},
            device_id_type=pl.DeviceIdType.MESH,
        )
    pl.semaphore_wait(barrier, 1 + tp_count)

    def landing(unit, source):
        if unit < 2:
            return gu_all.at[unit, pl.ds(pl.multiple_of(source * rows, rows), rows), :]
        return dn_all.at[
            source // 2, pl.ds((unit - 2) * half, half),
            pl.ds(pl.multiple_of((source % 2) * down_rows, down_rows), down_rows), :,
        ]

    def message(way, step, unit):
        source = index_at(1 - step if way == 0 else step - 1)
        place_of = landing(unit, source)
        if step == 1:
            src = gu_ref.at[unit] if unit < 2 else dn_ref.at[pl.ds((unit - 2) * half, half)]
        else:
            src = place_of
        return pltpu.make_async_remote_copy(
            src_ref=src, dst_ref=place_of,
            send_sem=send_sem.at[way, step - 1, unit], recv_sem=recv_sem.at[way, step - 1, unit],
            device_id={"fs": right if way == 0 else left},
            device_id_type=pl.DeviceIdType.MESH,
        )

    started = []

    def send(way, step, unit):
        if step < last or (step == last and unit % 2 == way):
            message(way, step, unit).start()
            started.append((way, step, unit))

    def receive(way, step, unit):
        if step < last or (step == last and unit % 2 == way):
            source = index_at(-step if way == 0 else step)
            place_of = landing(unit, source)
            pltpu.make_async_remote_copy(
                src_ref=place_of, dst_ref=place_of,
                send_sem=send_sem.at[way, step - 1, unit],
                recv_sem=recv_sem.at[way, step - 1, unit],
                device_id={"fs": right if way == 0 else left},
                device_id_type=pl.DeviceIdType.MESH,
            ).wait_recv()

    def relay(step, unit):
        for way in (0, 1):
            receive(way, step, unit)
            if step < last:
                send(way, step + 1, unit)

    for unit in (0, 1):
        for way in (0, 1):
            send(way, 1, unit)
    own = [
        pltpu.make_async_copy(gu_ref.at[unit], landing(unit, fs_at), own_sem.at[unit])
        for unit in (0, 1)
    ] + [
        pltpu.make_async_copy(
            dn_ref.at[pl.ds((unit - 2) * half, half)], landing(unit, fs_at), own_sem.at[unit]
        )
        for unit in (2, 3)
    ]
    for copy in own:
        copy.start()

    serves = []

    def serve(step):
        source = index_at(step)
        to = source // 2
        src = dn_all.at[
            source // 2, fs_at,
            pl.ds(pl.multiple_of((source % 2) * down_rows, down_rows), down_rows), :,
        ]
        dst = serve_ref.at[
            pl.ds(pl.multiple_of((source % 2) * down_rows, down_rows), down_rows),
            pl.ds(pl.multiple_of(tp_at * down_cols, down_cols), down_cols),
        ]
        slot = len(serves)
        remote = pltpu.make_async_remote_copy(
            src_ref=src, dst_ref=dst, send_sem=serve_send.at[slot],
            recv_sem=serve_recv.at[source % 2, tp_at],
            device_id={"tp": to}, device_id_type=pl.DeviceIdType.MESH,
        )
        local = pltpu.make_async_copy(src, dst, serve_copy.at[slot])
        pl.when(to != tp_at)(remote.start)
        pl.when(to == tp_at)(local.start)
        serves.append((to, remote, local))

    for step in range(1, last):
        for unit in (0, 1):
            relay(step, unit)
    for unit in (2, 3):
        for way in (0, 1):
            send(way, 1, unit)
    for copy in own:
        copy.wait()
    serve(0)
    for unit in (0, 1):
        relay(last, unit)

    lane = lax.broadcasted_iota(jnp.int32, (1, 384), 1)
    parity = jnp.where(lane < 256, lane // 128, (lane - 256) // 64)
    low = lax.broadcasted_iota(jnp.int32, (1, 128), 1) < 64
    height = tok_rows // blocks
    picks = []

    def evaluate(block):
        at = block * height
        tokens = normed_ref[pl.ds(at, height), :]
        ids = [ids_ref[pl.ds(at, height), pl.ds(k, 1)] for k in (0, 1)]
        folded = [jnp.zeros((height, 384), jnp.float32) for _ in (0, 1)]
        for first in range(0, half, 2):
            span = pl.ds(first * 384, 768)
            gate = jnp.dot(tokens, gu_all[0, :, span], preferred_element_type=jnp.float32)
            up = jnp.dot(tokens, gu_all[1, :, span], preferred_element_type=jnp.float32)
            hidden = gate / (1.0 + jnp.exp(-gate)) * up
            for pair in (0, 1):
                part = hidden[:, pair * 384 : (pair + 1) * 384]
                named = 2 * (first + pair) + parity
                for k in (0, 1):
                    folded[k] = folded[k] + jnp.where(ids[k] == named, part, 0.0)
        folded = [folded[k] * shares_ref[pl.ds(at, height), pl.ds(k, 1)] for k in (0, 1)]
        ends = [f[:, 256:384] + pltpu.roll(f[:, 256:384], 64, 1) for f in folded]
        for k in (0, 1):
            main = folded[k][:, :128] + folded[k][:, 128:256]
            picked[pl.ds(at, height), pl.ds(k * 128, 128)] = main.astype(jnp.bfloat16)
        picked[pl.ds(at, height), pl.ds(256, 128)] = jnp.where(low, ends[0], ends[1]).astype(
            jnp.bfloat16
        )
        for hop in range(1, tp_count):
            copy = pltpu.make_async_remote_copy(
                src_ref=picked.at[pl.ds(at, height), :],
                dst_ref=picked_all.at[tp_at, pl.ds(at, height), :],
                send_sem=pick_send.at[hop - 1, block], recv_sem=pick_recv.at[hop - 1, block],
                device_id={"tp": (tp_at + hop) % tp_count},
                device_id_type=pl.DeviceIdType.MESH,
            )
            copy.start()
            picks.append(copy)
        picked_all[tp_at, pl.ds(at, height), :] = picked[pl.ds(at, height), :]

    events = [(step, unit) for step in range(1, last) for unit in (2, 3)]

    def event():
        step, unit = events.pop(0)
        relay(step, unit)
        if unit == 3:
            serve(-step)
            serve(step)

    for block in range(blocks):
        evaluate(block)
        if block > 0:
            event()

    main_at = pl.multiple_of((fs_at // 2) * 384 + (fs_at % 2) * 128, 128)
    tail_at = pl.multiple_of((fs_at // 2) * 384 + 256, 128)
    main_ref[...] = gu_all[:, :, pl.ds(main_at, 128)]
    tail_ref[...] = gu_all[:, :, pl.ds(tail_at, 128)]

    while events:
        event()
    for hop in range(1, tp_count):
        for block in range(blocks):
            picks[block * (tp_count - 1) + hop - 1].wait()

    def project(index, first):
        for block in range(blocks):
            at = block * height
            ids = [ids_ref[pl.ds(at, height), pl.ds(k, 1)] for k in (0, 1)]
            held = picked_all[index, pl.ds(at, height), :].astype(jnp.float32)
            end = held[:, 256:384]
            turned = pltpu.roll(end, 64, 1)
            ends = [jnp.where(low, end, turned), jnp.where(low, turned, end)]
            pieces, weights = [], []
            for pair in range(half):
                for e in (2 * pair, 2 * pair + 1):
                    pieces.append(
                        jnp.where(ids[0] == e, held[:, :128],
                                  jnp.where(ids[1] == e, held[:, 128:256], 0.0))
                    )
                    weights.append(dn_all[index, e, pl.ds(0, 128), :])
                named = 2 * pair + parity[:, 256:384]
                pieces.append(
                    jnp.where(ids[0] == named, ends[0], jnp.where(ids[1] == named, ends[1], 0.0))
                )
                for e in (2 * pair, 2 * pair + 1):
                    weights.append(dn_all[index, e, pl.ds(128, 64), :])
            spread = jnp.concatenate([p.astype(jnp.bfloat16) for p in pieces], axis=1)
            product = jnp.dot(
                spread, jnp.concatenate(weights, axis=0), preferred_element_type=jnp.float32
            )
            if first:
                total[pl.ds(at, height), :] = product
            else:
                total[pl.ds(at, height), :] += product

    far = index_at(last) // 2
    project((far + 1) % last, True)

    def middle(step, carry):
        project((far + step) % last, False)
        return carry

    lax.fori_loop(2, last, middle, 0)
    for unit in (2, 3):
        relay(last, unit)
    serve(last)
    project(far, False)
    mixed_ref[...] = total[...].astype(jnp.bfloat16)

    for way, step, unit in started:
        message(way, step, unit).wait_send()
    for to, remote, local in serves:
        pl.when(to != tp_at)(remote.wait_send)
        pl.when(to == tp_at)(local.wait)
    for part in (0, 1):
        for source in range(tp_count):
            dst = serve_ref.at[
                pl.ds(part * down_rows, down_rows), pl.ds(source * down_cols, down_cols)
            ]
            arrival = pltpu.make_async_remote_copy(
                src_ref=dst, dst_ref=dst, send_sem=serve_send.at[0],
                recv_sem=serve_recv.at[part, source],
                device_id={"tp": (tp_at + 1) % tp_count}, device_id_type=pl.DeviceIdType.MESH,
            )
            pl.when(tp_at != source)(arrival.wait_recv)


def ringed(tokens, norm_gain, gate_train, up_train, down_train, expert_ids, route_weights):
    experts, rows, cols = gate_train.shape
    down_rows, down_cols = down_train.shape[1:]
    n, tp_count = lax.axis_size("fs"), lax.axis_size("tp")
    tok_rows, width = tokens.shape
    half = experts // 2
    blocks = 4

    def paired(train):
        value = (norm_gain[None, :, None] * train).astype(jnp.bfloat16)
        value = value.transpose(1, 0, 2).reshape(rows, half, 2, cols)
        return jnp.concatenate(
            [value[..., :128].reshape(rows, half, 256), value[..., 128:].reshape(rows, half, 128)],
            axis=2,
        ).reshape(rows, half * 384)

    tok_float = tokens.astype(jnp.float32)
    normed = (
        tok_float * lax.rsqrt(jnp.mean(tok_float * tok_float, axis=-1, keepdims=True) + epsilon)
    ).astype(jnp.bfloat16)
    shares = route_weights / jnp.sum(route_weights, axis=-1, keepdims=True)
    vmem = pl.BlockSpec(memory_space=pltpu.VMEM)
    dma = pltpu.SemaphoreType.DMA
    main, tail, serve, mixed = pl.pallas_call(
        functools.partial(ring_kernel, n, tp_count, blocks),
        out_shape=(
            jax.ShapeDtypeStruct((2, width, 128), jnp.bfloat16),
            jax.ShapeDtypeStruct((2, width, 128), jnp.bfloat16),
            jax.ShapeDtypeStruct((2 * down_rows, width), jnp.bfloat16),
            jax.ShapeDtypeStruct((tok_rows, down_cols), jnp.bfloat16),
        ),
        in_specs=[vmem] * 5,
        out_specs=(vmem,) * 4,
        scratch_shapes=[
            pltpu.VMEM((2, width, half * 384), jnp.bfloat16),
            pltpu.VMEM((n // 2, experts, 2 * down_rows, down_cols), jnp.bfloat16),
            pltpu.VMEM((tok_rows, 384), jnp.bfloat16),
            pltpu.VMEM((tp_count, tok_rows, 384), jnp.bfloat16),
            pltpu.VMEM((tok_rows, down_cols), jnp.float32),
            dma((2, n // 2, 4)),
            dma((2, n // 2, 4)),
            dma((tp_count - 1, blocks)),
            dma((tp_count - 1, blocks)),
            dma((n,)),
            dma((2, tp_count)),
            dma((n,)),
            dma((4,)),
        ],
        compiler_params=pltpu.CompilerParams(
            collective_id=0, has_side_effects=True, vmem_limit_bytes=60 * 1024 * 1024
        ),
    )(
        jnp.stack([paired(gate_train), paired(up_train)]), down_train.astype(jnp.bfloat16),
        normed, expert_ids, shares,
    )
    odd = lax.axis_index("fs") % 2
    whole = jnp.concatenate(
        [main, jnp.where(odd == 1, tail[..., 64:], tail[..., :64])], axis=2
    )
    return whole[0:1], whole[1:2], serve[None], mixed


def on_device(tokens, norm_gain, gate_train, up_train, down_train, expert_ids, route_weights):
    experts, rows, cols = gate_train.shape
    n, tp_count = lax.axis_size("fs"), lax.axis_size("tp")
    fits = experts == n and n == 2 * tp_count and cols == 192 and expert_ids.shape[1] == 2
    held = 3 * experts * n * rows * cols * 2
    run = ringed if fits and held < 24 * 1024 * 1024 else gathered
    return run(
        tokens, norm_gain, gate_train, up_train, down_train, expert_ids, route_weights
    )


def solution(mesh):
    return jax.shard_map(
        on_device,
        mesh=mesh,
        in_specs=(
            P("fs", None),
            P("fs"),
            P(None, "fs", "tp"),
            P(None, "fs", "tp"),
            P(None, "fs", "tp"),
            P("fs", None),
            P("fs", None),
        ),
        out_specs=(P("fs", None, "tp"), P("fs", None, "tp"), P("fs", "tp", None), P("fs", "tp")),
        check_vma=False,
    )
```

```python
import functools

import jax
import jax.numpy as jnp
from jax import lax
from jax.experimental import pallas as pl
from jax.experimental.pallas import tpu as pltpu
from jax.sharding import PartitionSpec as P

epsilon = 1e-06


def gathered(tokens, norm_gain, gate_train, up_train, down_train, expert_ids, route_weights):
    experts, rows, cols = gate_train.shape
    fs_at = lax.axis_index("fs")
    tok_rows, picks = expert_ids.shape
    down_rows, down_cols = down_train.shape[1:]
    fs_count = lax.axis_size("fs")

    gate_up = jnp.concatenate(
        [norm_gain[None, :, None] * gate_train, norm_gain[None, :, None] * up_train], axis=2
    ).astype(jnp.bfloat16)
    gate_up = gate_up.transpose(1, 0, 2).reshape(rows, experts * 2 * cols)
    gate_up_all = lax.all_gather(gate_up, "fs", axis=0, tiled=True)
    down_all = lax.all_gather(
        down_train.astype(jnp.bfloat16).reshape(experts * down_rows, down_cols),
        "fs", axis=0, tiled=True,
    )

    tok_float = tokens.astype(jnp.float32)
    normed = (
        tok_float * lax.rsqrt(jnp.mean(tok_float * tok_float, axis=-1, keepdims=True) + epsilon)
    ).astype(jnp.bfloat16)
    shares = route_weights / jnp.sum(route_weights, axis=-1, keepdims=True)

    group = 2 * lax.axis_size("tp")
    picked = [jnp.zeros((tok_rows, cols), jnp.float32) for _ in range(picks)]
    for first in range(0, experts, group):
        part = gate_up_all[:, first * 2 * cols : (first + group) * 2 * cols]
        if first:
            part, picked = lax.optimization_barrier((part, picked))
        acts = jnp.dot(normed, part, preferred_element_type=jnp.float32)
        for at in range(group):
            g = acts[:, at * 2 * cols : at * 2 * cols + cols]
            u = acts[:, at * 2 * cols + cols : (at + 1) * 2 * cols]
            h = jax.nn.silu(g) * u
            for k in range(picks):
                picked[k] = picked[k] + jnp.where(
                    expert_ids[:, k : k + 1] == first + at, h, 0.0
                )
    hidden = jnp.stack([picked[k] * shares[:, k : k + 1] for k in range(picks)], 0)
    hidden_all = lax.all_gather(hidden.astype(jnp.bfloat16), "tp", axis=2, tiled=True)
    hidden_all = hidden_all.reshape(picks, tok_rows, fs_count, 1, down_rows)
    ids = jnp.arange(experts, dtype=jnp.int32)[None, None, :, None]
    mixed = jnp.zeros((tok_rows, down_cols), jnp.float32)
    for first in range(0, fs_count, group):
        blocks = hidden_all[:, :, first : first + group]
        if first:
            blocks, mixed = lax.optimization_barrier((blocks, mixed))
        spread = jnp.zeros((tok_rows, group, experts, down_rows), jnp.bfloat16)
        for k in range(picks):
            spread = jnp.where(expert_ids[:, k][:, None, None, None] == ids, blocks[k], spread)
        depth = experts * down_rows
        mixed = mixed + jnp.dot(
            spread.reshape(tok_rows, group * depth),
            down_all[first * depth : (first + group) * depth],
            preferred_element_type=jnp.float32,
        )
    mixed = mixed.astype(jnp.bfloat16)

    own = lax.dynamic_slice_in_dim(gate_up_all, fs_at * 2 * cols, 2 * cols, 1)
    down_own = lax.dynamic_slice_in_dim(
        down_all.reshape(fs_count, experts, down_rows, down_cols), fs_at, 1, 1
    ).reshape(1, fs_count * down_rows, down_cols)
    down_serve = lax.all_to_all(down_own, "tp", split_axis=1, concat_axis=2, tiled=True)
    return own[None, :, :cols], own[None, :, cols:], down_serve, mixed


def ring_kernel(
    n, tp_count, blocks, gu_ref, dn_ref, tokens_ref, ids_ref, routes_ref,
    main_ref, tail_ref, serve_ref, mixed_ref,
    gu_all, dn_all, picked, picked_all, total,
    send_sem, recv_sem, pick_send, pick_recv, serve_send, serve_recv, serve_copy, own_sem,
):
    fs_at, tp_at = lax.axis_index("fs"), lax.axis_index("tp")
    experts, down_rows, down_cols = dn_ref.shape
    rows = gu_ref.shape[1]
    tok_rows = tokens_ref.shape[0]
    half = experts // 2
    last = n // 2

    place = (1 - fs_at % 2) * (fs_at // 2) + (fs_at % 2) * (n - 1 - fs_at // 2)

    def index_at(step):
        at = (place + step + n) % n
        odd = at // last
        return (1 - odd) * (2 * at) + odd * (2 * (n - 1 - at) + 1)

    right, left = index_at(1), index_at(-1)
    barrier = pltpu.get_barrier_semaphore()
    for to in (right, left):
        pl.semaphore_signal(
            barrier, inc=1, device_id={"fs": to}, device_id_type=pl.DeviceIdType.MESH
        )
    for hop in range(1, tp_count):
        pl.semaphore_signal(
            barrier, inc=1, device_id={"tp": (tp_at + hop) % tp_count},
            device_id_type=pl.DeviceIdType.MESH,
        )
    pl.semaphore_wait(barrier, 1 + tp_count)

    def landing(unit, source):
        if unit < 2:
            return gu_all.at[unit, pl.ds(pl.multiple_of(source * rows, rows), rows), :]
        return dn_all.at[
            source // 2, pl.ds((unit - 2) * half, half),
            pl.ds(pl.multiple_of((source % 2) * down_rows, down_rows), down_rows), :,
        ]

    def message(way, step, unit):
        source = index_at(1 - step if way == 0 else step - 1)
        place_of = landing(unit, source)
        if step == 1:
            src = gu_ref.at[unit] if unit < 2 else dn_ref.at[pl.ds((unit - 2) * half, half)]
        else:
            src = place_of
        return pltpu.make_async_remote_copy(
            src_ref=src, dst_ref=place_of,
            send_sem=send_sem.at[way, step - 1, unit], recv_sem=recv_sem.at[way, step - 1, unit],
            device_id={"fs": right if way == 0 else left},
            device_id_type=pl.DeviceIdType.MESH,
        )

    started = []

    def send(way, step, unit):
        if step < last or (step == last and unit % 2 == way):
            message(way, step, unit).start()
            started.append((way, step, unit))

    def receive(way, step, unit):
        if step < last or (step == last and unit % 2 == way):
            source = index_at(-step if way == 0 else step)
            place_of = landing(unit, source)
            pltpu.make_async_remote_copy(
                src_ref=place_of, dst_ref=place_of,
                send_sem=send_sem.at[way, step - 1, unit],
                recv_sem=recv_sem.at[way, step - 1, unit],
                device_id={"fs": right if way == 0 else left},
                device_id_type=pl.DeviceIdType.MESH,
            ).wait_recv()

    def relay(step, unit):
        for way in (0, 1):
            receive(way, step, unit)
            if step < last:
                send(way, step + 1, unit)

    for unit in (0, 1):
        for way in (0, 1):
            send(way, 1, unit)
    own = [
        pltpu.make_async_copy(gu_ref.at[unit], landing(unit, fs_at), own_sem.at[unit])
        for unit in (0, 1)
    ] + [
        pltpu.make_async_copy(
            dn_ref.at[pl.ds((unit - 2) * half, half)], landing(unit, fs_at), own_sem.at[unit]
        )
        for unit in (2, 3)
    ]
    for copy in own:
        copy.start()

    serves = []

    def serve(step):
        source = index_at(step)
        to = source // 2
        src = dn_all.at[
            source // 2, fs_at,
            pl.ds(pl.multiple_of((source % 2) * down_rows, down_rows), down_rows), :,
        ]
        dst = serve_ref.at[
            pl.ds(pl.multiple_of((source % 2) * down_rows, down_rows), down_rows),
            pl.ds(pl.multiple_of(tp_at * down_cols, down_cols), down_cols),
        ]
        slot = len(serves)
        remote = pltpu.make_async_remote_copy(
            src_ref=src, dst_ref=dst, send_sem=serve_send.at[slot],
            recv_sem=serve_recv.at[source % 2, tp_at],
            device_id={"tp": to}, device_id_type=pl.DeviceIdType.MESH,
        )
        local = pltpu.make_async_copy(src, dst, serve_copy.at[slot])
        pl.when(to != tp_at)(remote.start)
        pl.when(to == tp_at)(local.start)
        serves.append((to, remote, local))

    for step in range(1, last):
        for unit in (0, 1):
            relay(step, unit)
    for unit in (2, 3):
        for way in (0, 1):
            send(way, 1, unit)
    for copy in own:
        copy.wait()
    serve(0)
    for unit in (0, 1):
        relay(last, unit)

    lane = lax.broadcasted_iota(jnp.int32, (1, 384), 1)
    parity = jnp.where(lane < 256, lane // 128, (lane - 256) // 64)
    low = lax.broadcasted_iota(jnp.int32, (1, 128), 1) < 64
    height = tok_rows // blocks
    picks = []

    def evaluate(block):
        at = block * height
        tokens = tokens_ref[pl.ds(at, height), :].astype(jnp.float32)
        square = jnp.mean(tokens * tokens, axis=-1, keepdims=True)
        tokens = (tokens * lax.rsqrt(square + epsilon)).astype(jnp.bfloat16)
        ids = [ids_ref[pl.ds(at, height), pl.ds(k, 1)] for k in (0, 1)]
        folded = [jnp.zeros((height, 384), jnp.float32) for _ in (0, 1)]
        for first in range(0, half, 2):
            span = pl.ds(first * 384, 768)
            gate = jnp.dot(tokens, gu_all[0, :, span], preferred_element_type=jnp.float32)
            up = jnp.dot(tokens, gu_all[1, :, span], preferred_element_type=jnp.float32)
            hidden = gate / (1.0 + jnp.exp(-gate)) * up
            for pair in (0, 1):
                part = hidden[:, pair * 384 : (pair + 1) * 384]
                named = 2 * (first + pair) + parity
                for k in (0, 1):
                    folded[k] = folded[k] + jnp.where(ids[k] == named, part, 0.0)
        routes = [routes_ref[pl.ds(at, height), pl.ds(k, 1)] for k in (0, 1)]
        folded = [folded[k] * (routes[k] / (routes[0] + routes[1])) for k in (0, 1)]
        ends = [f[:, 256:384] + pltpu.roll(f[:, 256:384], 64, 1) for f in folded]
        for k in (0, 1):
            main = folded[k][:, :128] + folded[k][:, 128:256]
            picked[pl.ds(at, height), pl.ds(k * 128, 128)] = main.astype(jnp.bfloat16)
        picked[pl.ds(at, height), pl.ds(256, 128)] = jnp.where(low, ends[0], ends[1]).astype(
            jnp.bfloat16
        )
        for hop in range(1, tp_count):
            copy = pltpu.make_async_remote_copy(
                src_ref=picked.at[pl.ds(at, height), :],
                dst_ref=picked_all.at[tp_at, pl.ds(at, height), :],
                send_sem=pick_send.at[hop - 1, block], recv_sem=pick_recv.at[hop - 1, block],
                device_id={"tp": (tp_at + hop) % tp_count},
                device_id_type=pl.DeviceIdType.MESH,
            )
            copy.start()
            picks.append(copy)
        picked_all[tp_at, pl.ds(at, height), :] = picked[pl.ds(at, height), :]

    events = [(step, unit) for step in range(1, last) for unit in (2, 3)]

    def event():
        step, unit = events.pop(0)
        relay(step, unit)
        if unit == 3:
            serve(-step)
            serve(step)

    for block in range(blocks):
        evaluate(block)
        if block > 0:
            event()

    main_at = pl.multiple_of((fs_at // 2) * 384 + (fs_at % 2) * 128, 128)
    tail_at = pl.multiple_of((fs_at // 2) * 384 + 256, 128)
    main_ref[...] = gu_all[:, :, pl.ds(main_at, 128)]
    tail_ref[...] = gu_all[:, :, pl.ds(tail_at, 128)]

    while events:
        event()
    for hop in range(1, tp_count):
        for block in range(blocks):
            picks[block * (tp_count - 1) + hop - 1].wait()

    def project(index, first):
        for block in range(blocks):
            at = block * height
            ids = [ids_ref[pl.ds(at, height), pl.ds(k, 1)] for k in (0, 1)]
            held = picked_all[index, pl.ds(at, height), :].astype(jnp.float32)
            end = held[:, 256:384]
            turned = pltpu.roll(end, 64, 1)
            ends = [jnp.where(low, end, turned), jnp.where(low, turned, end)]
            pieces, weights = [], []
            for pair in range(half):
                for e in (2 * pair, 2 * pair + 1):
                    pieces.append(
                        jnp.where(ids[0] == e, held[:, :128],
                                  jnp.where(ids[1] == e, held[:, 128:256], 0.0))
                    )
                    weights.append(dn_all[index, e, pl.ds(0, 128), :])
                named = 2 * pair + parity[:, 256:384]
                pieces.append(
                    jnp.where(ids[0] == named, ends[0], jnp.where(ids[1] == named, ends[1], 0.0))
                )
                for e in (2 * pair, 2 * pair + 1):
                    weights.append(dn_all[index, e, pl.ds(128, 64), :])
            spread = jnp.concatenate([p.astype(jnp.bfloat16) for p in pieces], axis=1)
            product = jnp.dot(
                spread, jnp.concatenate(weights, axis=0), preferred_element_type=jnp.float32
            )
            if first:
                total[pl.ds(at, height), :] = product
            else:
                total[pl.ds(at, height), :] += product

    far = index_at(last) // 2
    project((far + 1) % last, True)

    def middle(step, carry):
        project((far + step) % last, False)
        return carry

    lax.fori_loop(2, last, middle, 0)
    for unit in (2, 3):
        relay(last, unit)
    serve(last)
    project(far, False)
    mixed_ref[...] = total[...].astype(jnp.bfloat16)

    for way, step, unit in started:
        message(way, step, unit).wait_send()
    for to, remote, local in serves:
        pl.when(to != tp_at)(remote.wait_send)
        pl.when(to == tp_at)(local.wait)
    for part in (0, 1):
        for source in range(tp_count):
            dst = serve_ref.at[
                pl.ds(part * down_rows, down_rows), pl.ds(source * down_cols, down_cols)
            ]
            arrival = pltpu.make_async_remote_copy(
                src_ref=dst, dst_ref=dst, send_sem=serve_send.at[0],
                recv_sem=serve_recv.at[part, source],
                device_id={"tp": (tp_at + 1) % tp_count}, device_id_type=pl.DeviceIdType.MESH,
            )
            pl.when(tp_at != source)(arrival.wait_recv)


def ringed(tokens, norm_gain, gate_train, up_train, down_train, expert_ids, route_weights):
    experts, rows, cols = gate_train.shape
    down_rows, down_cols = down_train.shape[1:]
    n, tp_count = lax.axis_size("fs"), lax.axis_size("tp")
    tok_rows, width = tokens.shape
    half = experts // 2
    blocks = 4

    def paired(train):
        value = (norm_gain[None, :, None] * train).astype(jnp.bfloat16)
        value = value.transpose(1, 0, 2).reshape(rows, half, 2, cols)
        return jnp.concatenate(
            [value[..., :128].reshape(rows, half, 256), value[..., 128:].reshape(rows, half, 128)],
            axis=2,
        ).reshape(rows, half * 384)

    vmem = pl.BlockSpec(memory_space=pltpu.VMEM)
    dma = pltpu.SemaphoreType.DMA
    main, tail, serve, mixed = pl.pallas_call(
        functools.partial(ring_kernel, n, tp_count, blocks),
        out_shape=(
            jax.ShapeDtypeStruct((2, width, 128), jnp.bfloat16),
            jax.ShapeDtypeStruct((2, width, 128), jnp.bfloat16),
            jax.ShapeDtypeStruct((2 * down_rows, width), jnp.bfloat16),
            jax.ShapeDtypeStruct((tok_rows, down_cols), jnp.bfloat16),
        ),
        in_specs=[vmem] * 5,
        out_specs=(vmem,) * 4,
        scratch_shapes=[
            pltpu.VMEM((2, width, half * 384), jnp.bfloat16),
            pltpu.VMEM((n // 2, experts, 2 * down_rows, down_cols), jnp.bfloat16),
            pltpu.VMEM((tok_rows, 384), jnp.bfloat16),
            pltpu.VMEM((tp_count, tok_rows, 384), jnp.bfloat16),
            pltpu.VMEM((tok_rows, down_cols), jnp.float32),
            dma((2, n // 2, 4)),
            dma((2, n // 2, 4)),
            dma((tp_count - 1, blocks)),
            dma((tp_count - 1, blocks)),
            dma((n,)),
            dma((2, tp_count)),
            dma((n,)),
            dma((4,)),
        ],
        compiler_params=pltpu.CompilerParams(
            collective_id=0, has_side_effects=True, vmem_limit_bytes=60 * 1024 * 1024
        ),
    )(
        jnp.stack([paired(gate_train), paired(up_train)]), down_train.astype(jnp.bfloat16),
        tokens, expert_ids, route_weights,
    )
    odd = lax.axis_index("fs") % 2
    whole = jnp.concatenate(
        [main, jnp.where(odd == 1, tail[..., 64:], tail[..., :64])], axis=2
    )
    return whole[0:1], whole[1:2], serve[None], mixed


def on_device(tokens, norm_gain, gate_train, up_train, down_train, expert_ids, route_weights):
    experts, rows, cols = gate_train.shape
    n, tp_count = lax.axis_size("fs"), lax.axis_size("tp")
    fits = experts == n and n == 2 * tp_count and cols == 192 and expert_ids.shape[1] == 2
    held = 3 * experts * n * rows * cols * 2
    run = ringed if fits and held < 24 * 1024 * 1024 else gathered
    return run(
        tokens, norm_gain, gate_train, up_train, down_train, expert_ids, route_weights
    )


def solution(mesh):
    return jax.shard_map(
        on_device,
        mesh=mesh,
        in_specs=(
            P("fs", None),
            P("fs"),
            P(None, "fs", "tp"),
            P(None, "fs", "tp"),
            P(None, "fs", "tp"),
            P("fs", None),
            P("fs", None),
        ),
        out_specs=(P("fs", None, "tp"), P("fs", None, "tp"), P("fs", "tp", None), P("fs", "tp")),
        check_vma=False,
    )
```
